32 devices in a mesh: grp: 2 (over y), sp: 2 (over x), tp: 4 (over z), dp: 2 (over core).
Axes of the slice: x: 2, y: 2, z: 4, core: 2. Of those that a mesh axis runs over, the one named last changes fastest.
Arguments:
- latent: bfloat16 [4, 768, 2048], P(('grp', 'dp'), ('sp', 'tp')), parts along dimension 0, may hold values from -6 to 6
- cond: bfloat16 [4, 2048], P(('grp', 'dp')), parts along dimension 0, may hold values from -6 to 6
- context: bfloat16 [4, 256, 2048], P(('grp', 'dp'), 'sp'), parts along dimension 0, may hold values from -6 to 6
- cond_ctx: bfloat16 [2048], replicated, may hold values from -8 to 8
- w_shift: bfloat16 [2048, 2048], P('sp', 'tp'), may hold values from -0.125 to 0.125
- w_scale: bfloat16 [2048, 2048], P('sp', 'tp'), may hold values from -0.125 to 0.125
- w_gate: bfloat16 [2048, 2048], P('sp', 'tp'), may hold values from -0.125 to 0.125
- norm_gain: float32 [2048], replicated, may hold values from 0.1 to 1.9
- w_query: bfloat16 [2048, 1024], P(None, 'tp'), may hold values from -0.125 to 0.125
- w_key: bfloat16 [2048, 512], P(None, 'tp'), may hold values from -0.125 to 0.125
- w_value: bfloat16 [2048, 512], P(None, 'tp'), may hold values from -0.125 to 0.125
- query_gain: float32 [128], replicated, may hold values from 0.6 to 16
- key_gain: float32 [128], replicated, may hold values from 0.6 to 16
- ctx_lift: float32 [8], P('tp'), may hold values from -2 to 0.5
- out_gain: float32 [1024], replicated, may hold values from 0.1 to 1.9
- w_out: bfloat16 [1024, 2048], replicated, may hold values from -0.1875 to 0.1875
Outputs:
- result: bfloat16 [4, 768, 2048], P(('grp', 'dp'), ('sp', 'tp')), parts along dimension 0
The draws below stay inside these ranges and needn't reach their ends.
There are 2 independent parts, one for each index of `grp`. The reference program is written for one: setup_inputs(seed, part) draws one part's arguments, and reference() takes and returns one part's arrays. A program takes and returns all parts, laid end to end along the dimension named above; an argument that names none is the same for every part. Nothing has to cross between parts.
All inputs are finite; a program needn't handle non-finite values.
Results may differ from the reference program's by a relative error of at most 0.023.
The reference program's roundings to bfloat16 on the way count: a program that leaves them out, or rounds other values in their place, can miss the bound.
Values may be sent and summed in bfloat16 or wider, within the bound.
A program may use at most 64 MiB of HBM per device.

```python
import math
import jax
import jax.numpy as jnp
from jax import lax

D = 2048
HEADS = 8
KV_HEADS = 4
HEAD_DIM = 128
GRID_WIDTH = 64
TOK_DEV = 384
CONTEXT = 256
BATCH = 2
TOKENS = 768
N_SP = 2


def gain_common(key, role):
    logs = jax.random.uniform(jax.random.fold_in(key, role), (HEAD_DIM,), jnp.float32, jnp.log(0.6), jnp.log(2.2))
    base = jnp.exp(logs)
    return base


def draw_query_gain(key, part):
    return gain_common(key, 11)


def draw_key_gain(key, part):
    return gain_common(key, 12)


def level_of(own_key, extent, pieces, low, top_value):
    level, own = 1.0, jax.random.fold_in(own_key, 6)
    for dim, shards_of in pieces:
        heights = jnp.exp(jax.random.uniform(jax.random.fold_in(own, dim), (shards_of,), jnp.float32, low / len(pieces), top_value / len(pieces)))
        level = level * jnp.repeat(heights, extent[dim] // shards_of).reshape([-1 if axis == dim else 1 for axis in range(len(extent))])
    return level


def noise(stream_key, extent, scale, limit, cuts=(), kind=jnp.bfloat16):
    drawn = scale * jax.random.normal(stream_key, extent, jnp.float32)
    if cuts:
        drawn = drawn * level_of(stream_key, extent, cuts, -0.22, 0.18)
    return jnp.clip(drawn, -limit, limit).astype(kind)


def setup_inputs(seed: int = 0, part: int = 0) -> dict:
    keys = jax.random.split(jax.random.key(seed), 17)
    own_keys = jax.random.split(jax.random.fold_in(keys[16], part), 17)
    latent = noise(own_keys[0], (BATCH, TOKENS, D), 1.0, 6.0, ((0, 2), (1, 8)))
    cond = noise(own_keys[1], (BATCH, D), 1.0, 6.0, ((0, 2),))
    context = noise(own_keys[2], (BATCH, CONTEXT, D), 1.0, 6.0, ((0, 2), (1, 2)))
    cond_ctx = noise(keys[3], (D,), 2.0, 8.0)
    w_shift = noise(keys[4], (D, D), D ** -0.5, 0.125, ((0, 2), (1, 4)))
    w_scale = noise(keys[5], (D, D), D ** -0.5, 0.125, ((0, 2), (1, 4)))
    w_gate = noise(keys[6], (D, D), D ** -0.5, 0.125, ((0, 2), (1, 4)))
    norm_gain = jnp.clip(1.0 + 0.18 * jax.random.normal(keys[7], (D,), jnp.float32), 0.1, 1.9)
    w_query = noise(keys[8], (D, HEADS * HEAD_DIM), D ** -0.5, 0.125, ((1, 4),))
    w_key = noise(keys[9], (D, KV_HEADS * HEAD_DIM), D ** -0.5, 0.125, ((1, 4),))
    w_value = noise(keys[10], (D, KV_HEADS * HEAD_DIM), D ** -0.5, 0.125, ((1, 4),))
    query_gain = draw_query_gain(jax.random.fold_in(keys[16], 71), part)
    key_gain = draw_key_gain(jax.random.fold_in(keys[16], 71), part)
    ctx_lift = jnp.clip(-2.0 + 2.5 * jax.random.uniform(keys[13], (HEADS,), jnp.float32) ** level_of(keys[13], (HEADS,), ((0, 4),), -0.2, 0.2), -2.0, 0.5)
    out_gain = jnp.clip(1.0 + 0.18 * jax.random.normal(keys[14], (HEADS * HEAD_DIM,), jnp.float32), 0.1, 1.9)
    w_out = noise(keys[15], (HEADS * HEAD_DIM, D), (HEADS * HEAD_DIM) ** -0.5, 0.1875)
    return dict(latent=latent, cond=cond, context=context, cond_ctx=cond_ctx, w_shift=w_shift, w_scale=w_scale, w_gate=w_gate, norm_gain=norm_gain, w_query=w_query, w_key=w_key, w_value=w_value, query_gain=query_gain, key_gain=key_gain, ctx_lift=ctx_lift, out_gain=out_gain, w_out=w_out)


EPSILON = 1e-06

def rotate(vectors, positions):
    freqs = vectors.shape[-1] // 4
    grid_rows = (positions // GRID_WIDTH).astype(jnp.float32)
    grid_cols = (positions % GRID_WIDTH).astype(jnp.float32)
    inverse = 10000.0 ** (-jnp.arange(freqs, dtype=jnp.float32) / freqs)
    angles = jnp.stack([grid_rows[:, None] * inverse, grid_cols[:, None] * inverse], axis=1)
    cosine = jnp.cos(angles)[:, None]
    sine = jnp.sin(angles)[:, None]
    split = vectors.reshape(vectors.shape[:-1] + (2, 2, freqs))
    first = split[..., 0, :]
    second = split[..., 1, :]
    return jnp.stack([first * cosine - second * sine, second * cosine + first * sine], axis=-2).reshape(vectors.shape)

def head_norm(vectors, gain_vector):
    floats = vectors.astype(jnp.float32)
    return floats * lax.rsqrt(lax.optimization_barrier(jnp.mean(floats * floats, -1, keepdims=True)) + EPSILON) * gain_vector.astype(jnp.float32)

def modulated_norm(row_data, gain_vector, shift_row, scale_row):
    floats = row_data.astype(jnp.float32)
    normal = floats * lax.rsqrt(lax.optimization_barrier(jnp.mean(floats * floats, -1, keepdims=True)) + EPSILON)
    return (normal * gain_vector * (1.0 + scale_row) + shift_row).astype(jnp.bfloat16)

def reference(latent, cond, context, cond_ctx, w_shift, w_scale, w_gate, norm_gain, w_query, w_key, w_value, query_gain, key_gain, ctx_lift, out_gain, w_out):
    group = HEADS // KV_HEADS
    inputs = jax.nn.silu(jnp.concatenate([cond, cond_ctx[None]], 0).astype(jnp.float32)).astype(jnp.bfloat16)
    shift_all = jnp.dot(inputs, w_shift, preferred_element_type=jnp.float32)
    scale_all = jnp.dot(inputs, w_scale, preferred_element_type=jnp.float32)
    gate_all = jnp.dot(inputs, w_gate, preferred_element_type=jnp.float32)
    batch = latent.shape[0]
    positions = jnp.arange(TOKENS, dtype=jnp.int32)
    lift_table = (ctx_lift + math.log(TOKENS / CONTEXT)).reshape(KV_HEADS, group)
    factor = HEAD_DIM ** (-0.5)
    outputs = []
    for sample in range(batch):
        normed = modulated_norm(latent[sample], norm_gain, shift_all[sample], scale_all[sample])
        query_rows = jnp.dot(normed, w_query, preferred_element_type=jnp.float32).astype(jnp.bfloat16)
        key_rows = jnp.dot(normed, w_key, preferred_element_type=jnp.float32).astype(jnp.bfloat16)
        value_rows = jnp.dot(normed, w_value, preferred_element_type=jnp.float32).astype(jnp.bfloat16)
        query_rows = rotate(head_norm(query_rows.reshape(TOKENS, HEADS, HEAD_DIM), query_gain), positions).astype(jnp.bfloat16)
        query_rows = query_rows.reshape(TOKENS, KV_HEADS, group, HEAD_DIM)
        key_rows = rotate(head_norm(key_rows.reshape(TOKENS, KV_HEADS, HEAD_DIM), key_gain), positions).astype(jnp.bfloat16)
        value_rows = value_rows.reshape(TOKENS, KV_HEADS, HEAD_DIM)
        ctx_normed = modulated_norm(context[sample], norm_gain, shift_all[batch], scale_all[batch])
        ctx_key_rows = jnp.dot(ctx_normed, w_key, preferred_element_type=jnp.float32).astype(jnp.bfloat16)
        ctx_key_rows = head_norm(ctx_key_rows.reshape(CONTEXT, KV_HEADS, HEAD_DIM), key_gain).astype(jnp.bfloat16)
        ctx_value_rows = jnp.dot(ctx_normed, w_value, preferred_element_type=jnp.float32).astype(jnp.bfloat16)
        ctx_value_rows = ctx_value_rows.reshape(CONTEXT, KV_HEADS, HEAD_DIM)
        key_float = key_rows.astype(jnp.float32)
        value_float = value_rows.astype(jnp.float32)
        ctx_key_float = ctx_key_rows.astype(jnp.float32)
        ctx_value_float = ctx_value_rows.astype(jnp.float32)

        def attend(block_queries):
            query_float = block_queries.astype(jnp.float32)
            latent_scores = jnp.einsum('qkgd,nkd->kgqn', query_float, key_float) * factor
            ctx_scores = jnp.einsum('qkgd,nkd->kgqn', query_float, ctx_key_float) * factor + lift_table[:, :, None, None]
            highest = jnp.maximum(lax.optimization_barrier(jnp.max(latent_scores, -1)), lax.optimization_barrier(jnp.max(ctx_scores, -1)))[..., None]
            latent_exp = jnp.exp(latent_scores - highest)
            ctx_exp = jnp.exp(ctx_scores - highest)
            denominator = lax.optimization_barrier(jnp.sum(latent_exp, -1)) + lax.optimization_barrier(jnp.sum(ctx_exp, -1))
            latent_weights = latent_exp.astype(jnp.bfloat16).astype(jnp.float32)
            ctx_weights = ctx_exp.astype(jnp.bfloat16).astype(jnp.float32)
            summed = jnp.einsum('kgqn,nkd->qkgd', latent_weights, value_float) + jnp.einsum('kgqn,nkd->qkgd', ctx_weights, ctx_value_float)
            return (summed / jnp.transpose(denominator, (2, 0, 1))[..., None]).astype(jnp.bfloat16)
        blocks = query_rows.reshape(N_SP, TOK_DEV, KV_HEADS, group, HEAD_DIM)
        attended = lax.map(attend, blocks).reshape(TOKENS, HEADS * HEAD_DIM)
        att_normed = head_norm(attended, out_gain).astype(jnp.bfloat16)
        mixture = jnp.dot(att_normed, w_out, preferred_element_type=jnp.float32)
        outputs.append((latent[sample].astype(jnp.float32) + gate_all[sample] * mixture).astype(jnp.bfloat16))
    return jnp.stack(outputs)
```

```python
import functools
import math

import jax
import jax.numpy as jnp
import numpy as np
from jax import lax
from jax.experimental import pallas as pl
from jax.experimental.pallas import tpu as pltpu
from jax.sharding import PartitionSpec as P

HEAD_DIM = 128
GRID_WIDTH = 64
EPSILON = 1e-06
MESH = pl.DeviceIdType.MESH
F32 = jnp.float32
BF16 = jnp.bfloat16


def position_tables(count):
    freqs = HEAD_DIM // 4
    places = np.arange(count)
    inverse = 10000.0 ** (-np.arange(freqs) / freqs)
    rows = (places // GRID_WIDTH)[:, None] * inverse
    cols = (places % GRID_WIDTH)[:, None] * inverse
    angles = np.concatenate([rows, rows, cols, cols], 1)
    signs = np.concatenate([-np.ones(freqs), np.ones(freqs)] * 2)
    return np.stack([np.cos(angles), np.sin(angles) * signs]).astype(np.float32)


def ring_kernel(n_sp, n_tp, *refs):
    (latent_h, cond_h, context_h, cond_ctx_h, ws_h, wc_h, wg_h, gain_h, wq_h, wk_h, wv_h,
     qgain_h, kgain_h, lift_h, ogain_h, wout_h, table_h, out_ref,
     x_all, cond_v, cond_ctx_v, ctx_v, wmod, gain_v, wqkv, qgain_v, kgain_v, lift_v, ogain_v,
     wout_v, table_v, mod_send, mod_recv, kv_lat, kv_ctx, q_buf, att_send, att_recv,
     load_sem, ctx_flat, r_send, r_recv, l_send, l_recv, m_send, m_recv,
     k_send, k_recv, a_send, a_recv) = refs
    sp = lax.axis_index("sp")
    tp = lax.axis_index("tp")
    rows, width = x_all.shape[1:]
    ctx_rows = ctx_v.shape[0]
    in_rows, mod_cols = wmod.shape[1:]
    q_cols = wq_h.shape[1]
    group = q_cols // HEAD_DIM
    half = rows // 2
    small = half - half // 3
    spans = ((0, small), (small, half - small), (half, small), (half + small, half - small))

    loads = {
        "latent": (latent_h.at[0], x_all.at[tp]),
        "cond": (cond_h, cond_v),
        "cond_ctx": (cond_ctx_h, cond_ctx_v),
        "ws": (ws_h, wmod.at[0]),
        "wc": (wc_h, wmod.at[1]),
        "wg": (wg_h, wmod.at[2]),
        "ctx": (context_h.at[0], ctx_v),
        "gain": (gain_h, gain_v),
        "wk": (wk_h, wqkv.at[:, pl.ds(q_cols, HEAD_DIM)]),
        "wv": (wv_h, wqkv.at[:, pl.ds(q_cols + HEAD_DIM, HEAD_DIM)]),
        "wq": (wq_h, wqkv.at[:, pl.ds(0, q_cols)]),
        "kgain": (kgain_h, kgain_v),
        "qgain": (qgain_h, qgain_v),
        "table": (
            table_h.at[:, pl.ds(pl.multiple_of(sp * (n_tp * rows), n_tp * rows), n_tp * rows)],
            table_v,
        ),
        "lift": (lift_h, lift_v),
        "ogain": (ogain_h, ogain_v),
        "wout": (wout_h, wout_v),
    }
    copies = {}
    for place, (name, (src, dst)) in enumerate(loads.items()):
        copies[name] = pltpu.make_async_copy(src, dst, load_sem.at[place])
        copies[name].start()

    def ready(*names):
        for name in names:
            copies[name].wait()

    def peer(ds, dt):
        return {"sp": lax.rem(sp + ds, n_sp), "tp": lax.rem(tp + dt, n_tp)}

    others = [(ds, dt) for ds in range(n_sp) for dt in range(n_tp) if (ds, dt) != (0, 0)]
    barrier = pltpu.get_barrier_semaphore()
    for ds, dt in others:
        pl.semaphore_signal(barrier, inc=1, device_id=peer(ds, dt), device_id_type=MESH)
    pl.semaphore_wait(barrier, len(others))

    sent = []

    def remote(src, dst, send_sem, recv_sem, target):
        return pltpu.make_async_remote_copy(
            src_ref=src, dst_ref=dst, send_sem=send_sem, recv_sem=recv_sem,
            device_id=target, device_id_type=MESH,
        )

    def send(copy):
        copy.start()
        sent.append(copy)

    def ring_right(step, part):
        block = lax.rem(tp - (step - 1) + n_tp, n_tp)
        piece = x_all.at[block, pl.ds(*spans[part])]
        return remote(piece, piece, r_send.at[step - 1, part], r_recv.at[step - 1, part], peer(0, 1))

    def ring_left(step, part):
        block = lax.rem(tp + (step - 1), n_tp)
        piece = x_all.at[block, pl.ds(*spans[part])]
        return remote(
            piece, piece, l_send.at[step - 1, part], l_recv.at[step - 1, part], peer(0, n_tp - 1)
        )

    def right_parts(step):
        return (0, 1) if 2 * step == n_tp else (0, 1, 2, 3)

    def left_parts(step):
        return (2, 3) if 2 * step == n_tp else (2, 3, 0, 1)

    steps = n_tp // 2
    ready("latent")
    if steps:
        for part in range(2):
            send(ring_right(1, right_parts(1)[part]))
            send(ring_left(1, left_parts(1)[part]))

    ready("cond", "cond_ctx")
    begin = pl.multiple_of(sp * in_rows, in_rows)
    own = cond_v[:, pl.ds(begin, in_rows)].astype(F32)
    ctx_flat[...] = cond_ctx_v[...].astype(F32).reshape(1, width)
    own_ctx = ctx_flat[:, pl.ds(begin, in_rows)]
    own = own * jax.nn.sigmoid(own)
    own_ctx = own_ctx * jax.nn.sigmoid(own_ctx)
    row_id = lax.broadcasted_iota(jnp.int32, (8, in_rows), 0)
    partial_mod = jnp.zeros((8, mod_cols), F32)
    for place, name in enumerate(("ws", "wc", "wg")):
        stacked = jnp.where(row_id == 2 * place, own, 0.0)
        stacked = jnp.where(row_id == 2 * place + 1, own_ctx, stacked).astype(BF16)
        ready(name)
        partial_mod += jnp.dot(stacked, wmod[place], preferred_element_type=F32)
    mod_send[...] = partial_mod
    mod_recv[sp, tp] = partial_mod

    mods = {}
    for ds, dt in sorted(others, key=lambda pair: -min(pair[1], n_tp - pair[1])):
        place = ds * n_tp + dt
        mods[place] = remote(
            mod_send, mod_recv.at[sp, tp], m_send.at[place], m_recv.at[place], peer(ds, dt)
        )
        send(mods[place])
    if steps:
        for part in right_parts(1)[2:]:
            send(ring_right(1, part))
        for part in left_parts(1)[2:]:
            send(ring_left(1, part))

    waited = set()

    def arrive_right(step, part):
        if ("r", step, part) not in waited:
            waited.add(("r", step, part))
            ring_right(step, part).wait_recv()

    def arrive_left(step, part):
        if ("l", step, part) not in waited:
            waited.add(("l", step, part))
            ring_left(step, part).wait_recv()

    for step in range(1, steps):
        for part_r, part_l in zip(right_parts(step), left_parts(step)):
            if part_r in right_parts(step + 1):
                arrive_right(step, part_r)
                send(ring_right(step + 1, part_r))
            if part_l in left_parts(step + 1):
                arrive_left(step, part_l)
                send(ring_left(step + 1, part_l))

    for copy in mods.values():
        copy.wait_recv()
    total_mod = mod_recv[0]
    for place in range(1, n_sp):
        total_mod = total_mod + mod_recv[place]
    modulation = jnp.concatenate([total_mod[place] for place in range(n_tp)], 1)
    ready("gain")
    gain_row = gain_v[...]
    shift = modulation[0:1]
    weight = gain_row * (1.0 + modulation[2:3])
    ctx_shift = modulation[1:2]
    ctx_weight = gain_row * (1.0 + modulation[3:4])
    gate = modulation[4:5]

    def pre_norm(data, weight_row, shift_row):
        floats = data.astype(F32)
        inverse = lax.rsqrt(jnp.mean(floats * floats, -1, keepdims=True) + EPSILON)
        return (floats * inverse * weight_row + shift_row).astype(BF16)

    def head_norm(projected, gain_vector):
        floats = projected.astype(BF16).astype(F32)
        return floats * lax.rsqrt(jnp.mean(floats * floats, -1, keepdims=True) + EPSILON) * gain_vector

    quarter = HEAD_DIM // 4
    lane = lax.broadcasted_iota(jnp.int32, (1, HEAD_DIM), 1)
    first = lax.rem(lane, 2 * quarter) < quarter

    def rotate(vectors, cosine, sine):
        swapped = jnp.where(
            first, pltpu.roll(vectors, HEAD_DIM - quarter, 1), pltpu.roll(vectors, quarter, 1)
        )
        return vectors * cosine + swapped * sine

    shared = []

    def share(buffer, place):
        for ds in range(1, n_sp):
            copy = remote(
                buffer, buffer, k_send.at[place, ds], k_recv.at[place, ds],
                {"sp": lax.rem(sp + ds, n_sp)},
            )
            send(copy)
            shared.append(copy)

    ready("ctx", "wk", "wv", "kgain")
    kgain = kgain_v[...]
    ctx_kv = jnp.dot(
        pre_norm(ctx_v[...], ctx_weight, ctx_shift), wqkv[:, q_cols:], preferred_element_type=F32
    )
    kv_ctx[sp, :, :HEAD_DIM] = head_norm(ctx_kv[:, :HEAD_DIM], kgain).astype(BF16)
    kv_ctx[sp, :, HEAD_DIM:] = ctx_kv[:, HEAD_DIM:].astype(BF16)
    share(kv_ctx.at[sp], n_tp)

    ready("wq", "qgain", "table")
    qgain = qgain_v[...]

    def project(block, place, parts=((0, rows),), slot=0):
        count = sum(size for _, size in parts)
        normed = pre_norm(
            jnp.concatenate([x_all[block, pl.ds(*part)] for part in parts], 0), weight, shift
        )
        out = jnp.dot(normed, wqkv[...], preferred_element_type=F32)

        def places(which):
            return jnp.concatenate(
                [
                    table_v[which, pl.ds(pl.multiple_of(block * rows + start, 8), size)]
                    for start, size in parts
                ],
                0,
            )

        cosine, sine = places(0), places(1)
        key = rotate(head_norm(out[:, q_cols : q_cols + HEAD_DIM], kgain), cosine, sine)
        kv_lat[sp, block, pl.ds(slot, count), :HEAD_DIM] = key.astype(BF16)
        kv_lat[sp, block, pl.ds(slot, count), HEAD_DIM:] = out[:, q_cols + HEAD_DIM :].astype(BF16)
        share(kv_lat.at[sp, block, pl.ds(slot, count)], place)
        for head in range(group):
            query = head_norm(out[:, head * HEAD_DIM : (head + 1) * HEAD_DIM], qgain)
            query = rotate(query, cosine, sine).astype(BF16)
            begin = 0
            for start, size in parts:
                q_buf[block, pl.ds(head * rows + start, size)] = query[begin : begin + size]
                begin += size

    project(tp, 0)
    for step in range(1, steps):
        for part in right_parts(step):
            arrive_right(step, part)
        project(lax.rem(tp - step + n_tp, n_tp), n_tp - step)
        for part in left_parts(step):
            arrive_left(step, part)
        project(lax.rem(tp + step, n_tp), step)

    for copy in shared:
        copy.wait_recv()
    near_shared = len(shared)
    ready("lift")
    factor = HEAD_DIM ** (-0.5)
    ratio = math.log(n_tp * rows / ctx_rows)
    lifts = jnp.concatenate(
        [jnp.broadcast_to(lift_v[0:1, head : head + 1] + ratio, (rows, 1)) for head in range(group)], 0
    )
    contract = (((1,), (1,)), ((), ()))
    far = steps

    def block_at(offset):
        return lax.rem(tp + offset, n_tp)

    def latent_part(offsets, channels):
        return jnp.concatenate(
            [
                kv_lat[place, block_at(offset), :, channels]
                for place in range(n_sp)
                for offset in offsets
            ],
            0,
        )

    key_part = slice(0, HEAD_DIM)
    value_part = slice(HEAD_DIM, 2 * HEAD_DIM)

    def scores_of(query, keys):
        return lax.dot_general(query, keys, contract, preferred_element_type=F32) * factor

    near = [offset for offset in range(n_tp) if offset != far]
    ctx_count = n_sp * ctx_rows

    def attend_near(offset):
        query = q_buf[block_at(offset)]
        scores = scores_of(query, latent_part(near, key_part))
        ctx_scores = scores_of(query, kv_ctx[:, :, key_part].reshape(ctx_count, HEAD_DIM)) + lifts
        highest = jnp.maximum(
            jnp.max(scores, -1, keepdims=True), jnp.max(ctx_scores, -1, keepdims=True)
        )
        weights = jnp.exp(scores - highest)
        ctx_weights = jnp.exp(ctx_scores - highest)
        total = jnp.sum(weights, -1, keepdims=True) + jnp.sum(ctx_weights, -1, keepdims=True)
        summed = jnp.dot(
            weights.astype(BF16), latent_part(near, value_part), preferred_element_type=F32
        ) + jnp.dot(
            ctx_weights.astype(BF16),
            kv_ctx[:, :, value_part].reshape(ctx_count, HEAD_DIM),
            preferred_element_type=F32,
        )
        return highest, total, summed

    def attend_far(offset, carried):
        highest, total, summed = carried
        scores = scores_of(q_buf[block_at(offset)], latent_part([far], key_part))
        topmost = jnp.maximum(highest, jnp.max(scores, -1, keepdims=True))
        keep = jnp.exp(highest - topmost)
        weights = jnp.exp(scores - topmost)
        total = total * keep + jnp.sum(weights, -1, keepdims=True)
        summed = summed * keep + jnp.dot(
            weights.astype(BF16), latent_part([far], value_part), preferred_element_type=F32
        )
        result = (summed / total).astype(BF16)
        return [result[head * rows : (head + 1) * rows] for head in range(group)]

    carried = {offset: attend_near(offset) for offset in near}
    for piece in range(2):
        arrive_right(steps, piece)
        arrive_left(steps, 2 + piece)
        parts = (spans[piece], spans[2 + piece])
        project(
            block_at(far), far if piece == 0 else n_tp + 1, parts, 0 if piece == 0 else 2 * small
        )
    carried[far] = attend_near(far)
    for copy in shared[near_shared:]:
        copy.wait_recv()

    returned = []
    for dt in sorted(range(1, n_tp), key=lambda d: -min(d, n_tp - d)):
        for head, piece in enumerate(attend_far(dt, carried[dt])):
            att_send[dt, :, head * HEAD_DIM : (head + 1) * HEAD_DIM] = piece
        copy = remote(
            att_send.at[dt], att_recv.at[tp], a_send.at[dt], a_recv.at[dt], {"tp": block_at(dt)}
        )
        send(copy)
        returned.append(copy)
    for head, piece in enumerate(attend_far(0, carried[0])):
        att_recv[tp, :, head * HEAD_DIM : (head + 1) * HEAD_DIM] = piece
    ready("ogain", "wout")
    for copy in returned:
        copy.wait_recv()

    tokens = jnp.concatenate([att_recv[place] for place in range(n_tp)], 1).astype(F32)
    inverse = lax.rsqrt(jnp.mean(tokens * tokens, -1, keepdims=True) + EPSILON)
    att_normed = (tokens * inverse * ogain_v[...]).astype(BF16)
    wide = width // 2
    for place in range(2):
        columns = slice(place * wide, (place + 1) * wide)
        mixture = jnp.dot(att_normed, wout_v[:, columns], preferred_element_type=F32)
        out_ref[0, :, columns] = (
            x_all[tp, :, columns].astype(F32) + gate[:, columns] * mixture
        ).astype(BF16)
    for copy in sent:
        copy.wait_send()


PARTS = 6
PIECES = ((0, 4), (4, 2))
SHARD_PIECES = 4


def line_kernel(*refs):
    (latent_h, cond_h, context_h, cond_ctx_h, ws_h, wc_h, wg_h, gain_h, wq_h, wk_h, wv_h,
     qgain_h, kgain_h, lift_h, ogain_h, wout_h, table_h, out_ref,
     x_all, cond_v, cond_ctx_v, ctx_v, wmod, gain_v, wqkv, wext, wshard, qgain_v, kgain_v,
     lift_v, ogain_v, wout_v, table_v, mod_send, mod_near, mod_sum, mod_all, kv_lat, kv_ctx,
     q_buf, q_ship, kv_ship, att_send, att_recv, ctx_flat,
     load_sem, token, near_s, in_s, x_recv, mx_s, mx_r, mz_s, mz_r, k_s, k_r, a_s, a_r,
     wz_s, wz_r, wx_s, wx_r, wy_s, wy_r, wc_s, wc_r, qs_s, qs_r, kvs_s, kvs_r) = refs
    n_tp = x_all.shape[0]
    n_sp = kv_lat.shape[0]
    sp = lax.axis_index("sp")
    tp = lax.axis_index("tp")
    grp = lax.axis_index("grp")
    dp = lax.axis_index("dp")
    rows, width = x_all.shape[1:]
    ctx_rows = ctx_v.shape[0]
    in_rows, mod_cols = wmod.shape[1:]
    q_cols = wq_h.shape[1]
    group = q_cols // HEAD_DIM
    part_rows = rows // PARTS
    shard_rows = wshard.shape[0]
    piece_rows = shard_rows // SHARD_PIECES

    half = lax.div(tp, 2)
    pair = tp + 1 - 2 * lax.rem(tp, 2)
    cross = n_tp // 2 - half
    hub = jnp.logical_or(tp == n_tp // 2 - 1, tp == n_tp // 2)
    edge = jnp.logical_not(hub)
    is_hub = hub.astype(jnp.int32)
    far_end = (n_tp - 1) * (1 - half)
    order = (
        tp,
        is_hub * cross + (1 - is_hub) * pair,
        is_hub * pair + (1 - is_hub) * cross,
        far_end,
    )

    shard_begin = pl.multiple_of(((sp * 2 + grp) * 2 + dp) * shard_rows, shard_rows)
    loads = {
        "latent": (latent_h.at[0], x_all.at[0]),
        "sq": (wq_h.at[pl.ds(shard_begin, shard_rows)], wshard.at[:, pl.ds(0, q_cols)]),
        "sk": (wk_h.at[pl.ds(shard_begin, shard_rows)], wshard.at[:, pl.ds(q_cols, HEAD_DIM)]),
        "sv": (
            wv_h.at[pl.ds(shard_begin, shard_rows)],
            wshard.at[:, pl.ds(q_cols + HEAD_DIM, HEAD_DIM)],
        ),
        "cond": (cond_h, cond_v),
        "cond_ctx": (cond_ctx_h, cond_ctx_v),
        "ws": (ws_h, wmod.at[0]),
        "wc": (wc_h, wmod.at[1]),
        "wg": (wg_h, wmod.at[2]),
        "ctx": (context_h.at[0], ctx_v),
        "gain": (gain_h, gain_v),
        "wk": (wk_h, wqkv.at[:, pl.ds(q_cols, HEAD_DIM)]),
        "wv": (wv_h, wqkv.at[:, pl.ds(q_cols + HEAD_DIM, HEAD_DIM)]),
        "wq": (wq_h, wqkv.at[:, pl.ds(0, q_cols)]),
        "kgain": (kgain_h, kgain_v),
        "qgain": (qgain_h, qgain_v),
        "table": (
            table_h.at[:, pl.ds(pl.multiple_of(sp * (n_tp * rows), n_tp * rows), n_tp * rows)],
            table_v,
        ),
        "lift": (lift_h, lift_v),
        "ogain": (ogain_h, ogain_v),
        "wout": (wout_h, wout_v),
    }
    copies = {}
    for place, (name, (src, dst)) in enumerate(loads.items()):
        copies[name] = pltpu.make_async_copy(src, dst, load_sem.at[place])
        copies[name].start()

    def ready(*names):
        for name in names:
            copies[name].wait()

    to_x = {"sp": 1 - sp}
    to_y = {"grp": 1 - grp}
    to_core = {"dp": 1 - dp}
    to_pair = {"tp": pair}
    to_cross = {"tp": cross}

    barrier = pltpu.get_barrier_semaphore()
    for target in (to_x, to_y, to_core, to_pair):
        pl.semaphore_signal(barrier, inc=1, device_id=target, device_id_type=MESH)

    @pl.when(hub)
    def _():
        pl.semaphore_signal(barrier, inc=1, device_id=to_cross, device_id_type=MESH)

    ready("latent", "sq", "sk", "sv")
    pl.semaphore_wait(barrier, 4 + is_hub)

    sent = []
    hub_sent = []
    edge_sent = []

    def remote(src, dst, send_sem, recv_sem, target):
        return pltpu.make_async_remote_copy(
            src_ref=src, dst_ref=dst, send_sem=send_sem, recv_sem=recv_sem,
            device_id=target, device_id_type=MESH,
        )

    def part_of(slot, part):
        return x_all.at[slot, pl.ds(part * part_rows, part_rows)]

    def raw(src_slot, dst_slot, part, send_sem, target):
        return remote(
            part_of(src_slot, part), part_of(dst_slot, part), send_sem,
            x_recv.at[dst_slot - 1, part], target,
        )

    def own_out(part):
        return raw(0, 1, part, near_s.at[0, part], to_pair)

    def own_up(part):
        return raw(0, 2, part, near_s.at[0, part], to_pair)

    def own_cross(part):
        return raw(0, 1, part, in_s.at[0, part], to_cross)

    def pass_cross(part):
        return raw(2, 3, part, in_s.at[1, part], to_cross)

    def pass_out(part):
        return raw(1, 2, part, near_s.at[1, part], to_pair)

    def arrive(slot, part):
        raw(0, slot, part, near_s.at[0, part], to_pair).wait_recv()

    def flip(index, other):
        return 1 - index if other else index

    def shard_piece(ds, dg, dc, piece):
        place = (flip(sp, ds) * 2 + flip(grp, dg)) * 2 + flip(dp, dc)
        return pl.ds(pl.multiple_of(place * shard_rows + piece * piece_rows, piece_rows), piece_rows)

    def w_up(piece):
        return remote(
            wshard.at[pl.ds(piece * piece_rows, piece_rows)], wext.at[shard_piece(0, 0, 0, piece)],
            wz_s.at[piece], wz_r.at[piece], to_pair,
        )

    def w_move(way, place, ds, dg, piece):
        send_sem, recv_sem, target = {
            "x": (wx_s, wx_r, to_x), "y": (wy_s, wy_r, to_y), "core": (wc_s, wc_r, to_core),
        }[way]
        block = wext.at[shard_piece(ds, dg, 0, piece)]
        return remote(block, block, send_sem.at[place], recv_sem.at[place], target)

    def start_all(group_of, store):
        for make, *given in group_of:
            make(*given).start()
            store.append((make, given))

    early = PARTS // 2

    @pl.when(edge)
    def _():
        start_all([(w_up, piece) for piece in range(3)], edge_sent)

    @pl.when(hub)
    def _():
        for part in range(early):
            start_all([(own_cross, part), (own_out, part)], hub_sent)
        pl.semaphore_signal(token, inc=1, device_id=to_cross, device_id_type=MESH)

    ready("cond", "cond_ctx")
    begin = pl.multiple_of(sp * in_rows, in_rows)
    own = cond_v[:, pl.ds(begin, in_rows)].astype(F32)
    ctx_flat[...] = cond_ctx_v[...].astype(F32).reshape(1, width)
    own_ctx = ctx_flat[:, pl.ds(begin, in_rows)]
    own = own * jax.nn.sigmoid(own)
    own_ctx = own_ctx * jax.nn.sigmoid(own_ctx)
    row_id = lax.broadcasted_iota(jnp.int32, (8, in_rows), 0)
    partial_mod = jnp.zeros((8, mod_cols), F32)
    for place, name in enumerate(("ws", "wc", "wg")):
        stacked = jnp.where(row_id == 2 * place, own, 0.0)
        stacked = jnp.where(row_id == 2 * place + 1, own_ctx, stacked).astype(BF16)
        ready(name)
        partial_mod += jnp.dot(stacked, wmod[place], preferred_element_type=F32)
    mod_send[...] = partial_mod
    across = remote(mod_send, mod_near, mx_s, mx_r, to_x)
    across.start()
    sent.append(across)
    across.wait_recv()
    total_mod = partial_mod + mod_near[...]
    mod_sum[...] = total_mod
    mod_all[tp] = total_mod

    pl.semaphore_wait(token, 1)

    @pl.when(hub)
    def _():
        pl.semaphore_signal(token, inc=1, device_id=to_pair, device_id_type=MESH)

    mods = []
    for dt in range(1, n_tp):
        copy = remote(
            mod_sum, mod_all.at[tp], mz_s.at[dt], mz_r.at[dt], {"tp": lax.rem(tp + dt, n_tp)}
        )
        copy.start()
        sent.append(copy)
        mods.append(copy)

    @pl.when(edge)
    def _():
        start_all([(w_up, piece) for piece in range(3, SHARD_PIECES)], edge_sent)
        start_all([(own_up, part) for part in range(PARTS)], edge_sent)

    @pl.when(hub)
    def _():
        for part in range(early, PARTS):
            start_all([(own_cross, part), (own_out, part)], hub_sent)
        for piece in range(SHARD_PIECES):
            w_up(piece).wait_recv()
            start_all(
                [
                    (w_move, "x", piece, 0, 0, piece),
                    (w_move, "y", piece, 0, 0, piece),
                    (w_move, "core", (0, piece), 0, 0, piece),
                ],
                hub_sent,
            )

    for copy in mods:
        copy.wait_recv()
    modulation = jnp.concatenate([mod_all[place] for place in range(n_tp)], 1)
    ready("gain")
    gain_row = gain_v[...]
    shift = modulation[0:1]
    weight = gain_row * (1.0 + modulation[2:3])
    ctx_shift = modulation[1:2]
    ctx_weight = gain_row * (1.0 + modulation[3:4])
    gate = modulation[4:5]

    def pre_norm(data, weight_row, shift_row):
        floats = data.astype(F32)
        inverse = lax.rsqrt(jnp.mean(floats * floats, -1, keepdims=True) + EPSILON)
        return (floats * inverse * weight_row + shift_row).astype(BF16)

    def head_norm(projected, gain_vector):
        floats = projected.astype(BF16).astype(F32)
        return floats * lax.rsqrt(jnp.mean(floats * floats, -1, keepdims=True) + EPSILON) * gain_vector

    quarter = HEAD_DIM // 4
    lane = lax.broadcasted_iota(jnp.int32, (1, HEAD_DIM), 1)
    first = lax.rem(lane, 2 * quarter) < quarter

    def rotate(vectors, cosine, sine):
        swapped = jnp.where(
            first, pltpu.roll(vectors, HEAD_DIM - quarter, 1), pltpu.roll(vectors, quarter, 1)
        )
        return vectors * cosine + swapped * sine

    def share(buffer, place):
        copy = remote(buffer, buffer, k_s.at[place], k_r.at[place], to_x)
        copy.start()
        return copy

    ready("ctx", "wk", "wv", "kgain")
    kgain = kgain_v[...]
    ctx_kv = jnp.dot(
        pre_norm(ctx_v[...], ctx_weight, ctx_shift), wqkv[:, q_cols:], preferred_element_type=F32
    )
    kv_ctx[sp, :, :HEAD_DIM] = head_norm(ctx_kv[:, :HEAD_DIM], kgain).astype(BF16)
    kv_ctx[sp, :, HEAD_DIM:] = ctx_kv[:, HEAD_DIM:].astype(BF16)
    shared = {"ctx": share(kv_ctx.at[sp], 0)}

    ready("wq", "qgain", "table")
    qgain = qgain_v[...]

    def finish(out, slot, start, count, q_dst, kv_dst):
        place = pl.multiple_of(order[slot] * rows + start, 8)
        cosine = table_v[0, pl.ds(place, count)]
        sine = table_v[1, pl.ds(place, count)]
        key = rotate(head_norm(out[:, q_cols : q_cols + HEAD_DIM], kgain), cosine, sine)
        kv_dst[:, :HEAD_DIM] = key.astype(BF16)
        kv_dst[:, HEAD_DIM:] = out[:, q_cols + HEAD_DIM :].astype(BF16)
        for head in range(group):
            query = head_norm(out[:, head * HEAD_DIM : (head + 1) * HEAD_DIM], qgain)
            q_dst[head] = rotate(query, cosine, sine).astype(BF16)

    def normed_rows(slot, start, count):
        return pre_norm(x_all[slot, pl.ds(start, count)], weight, shift)

    def project(normed, slot, start, count):
        finish(
            jnp.dot(normed, wqkv[...], preferred_element_type=F32), slot, start, count,
            q_buf.at[slot, :, pl.ds(start, count)], kv_lat.at[sp, slot, pl.ds(start, count)],
        )

    project(normed_rows(0, 0, rows), 0, 0, rows)
    shared[0] = share(kv_lat.at[sp, 0], 1)

    @pl.when(hub)
    def _():
        for part in range(PARTS):
            arrive(1, part)
            start_all([(pass_out, part)], hub_sent)
        for piece in range(SHARD_PIECES):
            w_move("x", piece, 0, 0, piece).wait_recv()
            w_move("y", piece, 0, 0, piece).wait_recv()
            start_all(
                [
                    (w_move, "core", (1, piece), 1, 0, piece),
                    (w_move, "core", (2, piece), 0, 1, piece),
                ],
                hub_sent,
            )
            spare = SHARD_PIECES + piece % 2
            if piece < SHARD_PIECES // 2:
                start_all([(w_move, "y", spare, 1, 0, piece)], hub_sent)
            else:
                start_all([(w_move, "x", spare, 0, 1, piece)], hub_sent)
        for part in range(2):
            arrive(2, part)
            start_all([(pass_cross, part)], hub_sent)

    @pl.when(edge)
    def _():
        for part in range(PARTS):
            arrive(1, part)

    project(normed_rows(1, 0, rows), 1, 0, rows)
    shared[1] = share(kv_lat.at[sp, 1], 2)

    @pl.when(hub)
    def _():
        for part in range(2, 4):
            arrive(2, part)
            start_all([(pass_cross, part)], hub_sent)

    for name in ("ctx", 0, 1):
        shared[name].wait_recv()
    ready("lift")
    factor = HEAD_DIM ** (-0.5)
    ratio = math.log(n_tp * rows / ctx_rows)
    contract = (((1,), (1,)), ((), ()))
    key_part = slice(0, HEAD_DIM)
    value_part = slice(HEAD_DIM, 2 * HEAD_DIM)
    ctx_count = n_sp * ctx_rows

    def scores_of(query, keys):
        return lax.dot_general(query, keys, contract, preferred_element_type=F32) * factor

    def latent_part(slots, channels):
        return jnp.concatenate(
            [kv_lat[place, slot, :, channels] for place in range(n_sp) for slot in slots], 0
        )

    def query_of(slot, start, count):
        return q_buf[slot, :, pl.ds(start, count)].reshape(group * count, HEAD_DIM)

    def attend_first(slot, start=0, count=rows):
        query = query_of(slot, start, count)
        lifts = jnp.concatenate(
            [
                jnp.broadcast_to(lift_v[0:1, head : head + 1] + ratio, (count, 1))
                for head in range(group)
            ],
            0,
        )
        scores = scores_of(query, latent_part((0, 1), key_part))
        ctx_scores = scores_of(query, kv_ctx[:, :, key_part].reshape(ctx_count, HEAD_DIM)) + lifts
        highest = jnp.maximum(
            jnp.max(scores, -1, keepdims=True), jnp.max(ctx_scores, -1, keepdims=True)
        )
        weights = jnp.exp(scores - highest)
        ctx_weights = jnp.exp(ctx_scores - highest)
        total = jnp.sum(weights, -1, keepdims=True) + jnp.sum(ctx_weights, -1, keepdims=True)
        summed = jnp.dot(
            weights.astype(BF16), latent_part((0, 1), value_part), preferred_element_type=F32
        ) + jnp.dot(
            ctx_weights.astype(BF16),
            kv_ctx[:, :, value_part].reshape(ctx_count, HEAD_DIM),
            preferred_element_type=F32,
        )
        return highest, total, summed

    def attend_more(carried, key_slot, slot, start=0, count=rows):
        highest, total, summed = carried
        scores = scores_of(query_of(slot, start, count), latent_part((key_slot,), key_part))
        topmost = jnp.maximum(highest, jnp.max(scores, -1, keepdims=True))
        keep = jnp.exp(highest - topmost)
        weights = jnp.exp(scores - topmost)
        total = total * keep + jnp.sum(weights, -1, keepdims=True)
        summed = summed * keep + jnp.dot(
            weights.astype(BF16), latent_part((key_slot,), value_part), preferred_element_type=F32
        )
        return topmost, total, summed

    carried = {0: attend_first(0)}

    @pl.when(hub)
    def _():
        for part in range(4, 5):
            arrive(2, part)
            start_all([(pass_cross, part)], hub_sent)

    carried[1] = attend_first(1)

    @pl.when(hub)
    def _():
        for part in range(5, PARTS):
            arrive(2, part)
            start_all([(pass_cross, part)], hub_sent)
        for piece in range(SHARD_PIECES):
            spare = SHARD_PIECES + piece % 2
            if piece < SHARD_PIECES // 2:
                w_move("y", spare, 1, 0, piece).wait_recv()
            else:
                w_move("x", spare, 0, 1, piece).wait_recv()
            start_all([(w_move, "core", (3, piece), 1, 1, piece)], hub_sent)

    @pl.when(edge)
    def _():
        for part in range(PARTS):
            arrive(2, part)

    project(normed_rows(2, 0, rows), 2, 0, rows)
    shared[2] = share(kv_lat.at[sp, 2], 3)
    carried[2] = attend_first(2)

    far_spans = [(begin * part_rows, count * part_rows) for begin, count in PIECES]

    def ship_query(piece):
        span = pl.ds(*far_spans[piece])
        return remote(
            q_ship.at[:, span], q_buf.at[3, :, span], qs_s.at[piece], qs_r.at[piece], to_pair
        )

    def ship_keys(piece, place):
        span = pl.ds(*far_spans[piece])
        target = {"sp": flip(sp, place), "tp": pair}
        return remote(
            kv_ship.at[span], kv_lat.at[sp, 3, span], kvs_s.at[piece, place],
            kvs_r.at[piece, place], target,
        )

    def far_share(piece):
        block = kv_lat.at[sp, 3, pl.ds(*far_spans[piece])]
        return remote(block, block, k_s.at[4 + piece], k_r.at[4 + piece], to_x)

    def far_piece(piece):
        start, count = far_spans[piece]
        begin, parts = PIECES[piece]

        @pl.when(hub)
        def _():
            for part in range(begin, begin + parts):
                arrive(3, part)
            if piece == 0:
                for shard in range(4):
                    for step in range(SHARD_PIECES):
                        w_move("core", (shard, step), 0, 0, step).wait_recv()
            normed = normed_rows(3, start, count)
            finish(
                jnp.dot(normed, wext[...], preferred_element_type=F32), 3, start, count,
                q_ship.at[:, pl.ds(start, count)], kv_ship.at[pl.ds(start, count)],
            )
            start_all(
                [(ship_keys, piece, 1), (ship_keys, piece, 0), (ship_query, piece)], hub_sent
            )
            project(normed, 3, start, count)
            start_all([(far_share, piece)], hub_sent)

    def far_wait(piece):
        @pl.when(hub)
        def _():
            far_share(piece).wait_recv()

        @pl.when(edge)
        def _():
            for place in range(n_sp):
                ship_keys(piece, place).wait_recv()

    def far_query_wait(piece):
        @pl.when(edge)
        def _():
            ship_query(piece).wait_recv()

    far_piece(0)
    shared[2].wait_recv()
    for slot in range(3):
        carried[slot] = attend_more(carried[slot], 2, slot)
    far_query_wait(0)
    far_carried = [attend_more(attend_first(3, *far_spans[0]), 2, 3, *far_spans[0])]
    far_piece(1)
    far_query_wait(1)
    far_carried.append(attend_more(attend_first(3, *far_spans[1]), 2, 3, *far_spans[1]))
    far_wait(0)
    far_wait(1)

    def ready_rows(carried_part, slot, start=0, count=rows):
        _, total, summed = attend_more(carried_part, 3, slot, start, count)
        result = (summed / total).astype(BF16)
        return [result[head * count : (head + 1) * count] for head in range(group)]

    def att_copy(slot, source):
        return remote(
            att_send.at[slot], att_recv.at[source], a_s.at[slot], a_r.at[source],
            {"tp": order[slot]},
        )

    def place_rows(dst, pieces, start=0, count=rows):
        for head, piece in enumerate(pieces):
            dst[pl.ds(start, count), head * HEAD_DIM : (head + 1) * HEAD_DIM] = piece

    returned = []
    for slot in (3, 2, 1):
        if slot == 3:
            for piece, span in enumerate(far_spans):
                place_rows(att_send.at[slot], ready_rows(far_carried[piece], 3, *span), *span)
        else:
            place_rows(att_send.at[slot], ready_rows(carried[slot], slot))
        copy = att_copy(slot, tp)
        copy.start()
        sent.append(copy)
        returned.append(att_copy(slot, order[slot]))
    place_rows(att_recv.at[tp], ready_rows(carried[0], 0))
    ready("ogain", "wout")
    for copy in returned:
        copy.wait_recv()

    tokens = jnp.concatenate([att_recv[place] for place in range(n_tp)], 1).astype(F32)
    inverse = lax.rsqrt(jnp.mean(tokens * tokens, -1, keepdims=True) + EPSILON)
    att_normed = (tokens * inverse * ogain_v[...]).astype(BF16)
    wide = width // 2
    for place in range(2):
        columns = slice(place * wide, (place + 1) * wide)
        mixture = jnp.dot(att_normed, wout_v[:, columns], preferred_element_type=F32)
        out_ref[0, :, columns] = (
            x_all[0, :, columns].astype(F32) + gate[:, columns] * mixture
        ).astype(BF16)
    sent.extend(shared.values())
    for copy in sent:
        copy.wait_send()

    @pl.when(hub)
    def _():
        for make, given in hub_sent:
            make(*given).wait_send()

    @pl.when(edge)
    def _():
        for make, given in edge_sent:
            make(*given).wait_send()


def line_call(operands):
    latent, context, w_shift, w_query, w_out = (operands[i] for i in (0, 2, 4, 8, 15))
    n_sp, n_tp, planes = 2, 4, 8
    rows, width = latent.shape[1:]
    ctx_rows = context.shape[1]
    in_rows, mod_cols = w_shift.shape
    q_cols = w_query.shape[1]
    group = q_cols // HEAD_DIM
    inner = w_out.shape[0]
    qkv_cols = q_cols + 2 * HEAD_DIM
    assert rows % (16 * PARTS) == 0 and width % (planes * SHARD_PIECES * 16) == 0
    dma = pltpu.SemaphoreType.DMA
    return pl.pallas_call(
        line_kernel,
        out_shape=pltpu.VMEM(latent.shape, BF16),
        in_specs=[pl.BlockSpec(memory_space=pl.ANY)] * len(operands),
        out_specs=pl.BlockSpec(memory_space=pltpu.VMEM),
        scratch_shapes=[
            pltpu.VMEM((n_tp, rows, width), BF16),
            pltpu.VMEM((1, width), BF16),
            pltpu.VMEM((width,), BF16),
            pltpu.VMEM((ctx_rows, width), BF16),
            pltpu.VMEM((3, in_rows, mod_cols), BF16),
            pltpu.VMEM((1, width), F32),
            pltpu.VMEM((width, qkv_cols), BF16),
            pltpu.VMEM((width, qkv_cols), BF16),
            pltpu.VMEM((width // planes, qkv_cols), BF16),
            pltpu.VMEM((1, HEAD_DIM), F32),
            pltpu.VMEM((1, HEAD_DIM), F32),
            pltpu.VMEM((1, group), F32),
            pltpu.VMEM((1, inner), F32),
            pltpu.VMEM((inner, width), BF16),
            pltpu.VMEM((2, n_tp * rows, HEAD_DIM), F32),
            pltpu.VMEM((8, mod_cols), F32),
            pltpu.VMEM((8, mod_cols), F32),
            pltpu.VMEM((8, mod_cols), F32),
            pltpu.VMEM((n_tp, 8, mod_cols), F32),
            pltpu.VMEM((n_sp, n_tp, rows, 2 * HEAD_DIM), BF16),
            pltpu.VMEM((n_sp, ctx_rows, 2 * HEAD_DIM), BF16),
            pltpu.VMEM((n_tp, group, rows, HEAD_DIM), BF16),
            pltpu.VMEM((group, rows, HEAD_DIM), BF16),
            pltpu.VMEM((rows, 2 * HEAD_DIM), BF16),
            pltpu.VMEM((n_tp, rows, q_cols), BF16),
            pltpu.VMEM((n_tp, rows, q_cols), BF16),
            pltpu.VMEM((1, width), F32),
            dma((len(operands) + 3,)),
            pltpu.SemaphoreType.REGULAR,
            dma((2, PARTS)),
            dma((2, PARTS)),
            dma((3, PARTS)),
            dma, dma,
            dma((n_tp,)),
            dma((n_tp,)),
            dma((6,)),
            dma((6,)),
            dma((n_tp,)),
            dma((n_tp,)),
            dma((SHARD_PIECES,)),
            dma((SHARD_PIECES,)),
            dma((SHARD_PIECES + 2,)),
            dma((SHARD_PIECES + 2,)),
            dma((SHARD_PIECES + 2,)),
            dma((SHARD_PIECES + 2,)),
            dma((4, SHARD_PIECES)),
            dma((4, SHARD_PIECES)),
            dma((2,)),
            dma((2,)),
            dma((2, n_sp)),
            dma((2, n_sp)),
        ],
        compiler_params=pltpu.CompilerParams(
            collective_id=0, has_side_effects=True, vmem_limit_bytes=60 * 2**20
        ),
    )(*operands)


def solution(mesh):
    n_sp, n_tp = mesh.shape["sp"], mesh.shape["tp"]
    planes = (mesh.shape["grp"], n_sp, mesh.shape["dp"])
    on_line = planes == (2, 2, 2) and n_tp == 4

    def on_device(latent, cond, context, cond_ctx, w_shift, w_scale, w_gate, norm_gain, w_query,
                  w_key, w_value, query_gain, key_gain, ctx_lift, out_gain, w_out):
        rows, width = latent.shape[1:]
        ctx_rows = context.shape[1]
        in_rows, mod_cols = w_shift.shape
        q_cols, k_cols = w_query.shape[1], w_key.shape[1]
        assert k_cols == HEAD_DIM and rows % 96 == 0 and n_tp % 2 == 0
        group = q_cols // HEAD_DIM
        inner = w_out.shape[0]
        table = jnp.asarray(position_tables(n_sp * n_tp * rows))
        steps = max(n_tp // 2, 1)
        operands = (
            latent, cond, context, cond_ctx, w_shift, w_scale, w_gate, norm_gain[None],
            w_query, w_key, w_value, query_gain[None], key_gain[None], ctx_lift[None],
            out_gain[None], w_out, table,
        )
        dma = pltpu.SemaphoreType.DMA
        if on_line:
            return line_call(operands)
        return pl.pallas_call(
            functools.partial(ring_kernel, n_sp, n_tp),
            out_shape=pltpu.VMEM(latent.shape, BF16),
            in_specs=[pl.BlockSpec(memory_space=pl.ANY)] * len(operands),
            out_specs=pl.BlockSpec(memory_space=pltpu.VMEM),
            scratch_shapes=[
                pltpu.VMEM((n_tp, rows, width), BF16),
                pltpu.VMEM((1, width), BF16),
                pltpu.VMEM((width,), BF16),
                pltpu.VMEM((ctx_rows, width), BF16),
                pltpu.VMEM((3, in_rows, mod_cols), BF16),
                pltpu.VMEM((1, width), F32),
                pltpu.VMEM((width, q_cols + 2 * HEAD_DIM), BF16),
                pltpu.VMEM((1, HEAD_DIM), F32),
                pltpu.VMEM((1, HEAD_DIM), F32),
                pltpu.VMEM((1, group), F32),
                pltpu.VMEM((1, inner), F32),
                pltpu.VMEM((inner, width), BF16),
                pltpu.VMEM((2, n_tp * rows, HEAD_DIM), F32),
                pltpu.VMEM((8, mod_cols), F32),
                pltpu.VMEM((n_sp, n_tp, 8, mod_cols), F32),
                pltpu.VMEM((n_sp, n_tp, rows, 2 * HEAD_DIM), BF16),
                pltpu.VMEM((n_sp, ctx_rows, 2 * HEAD_DIM), BF16),
                pltpu.VMEM((n_tp, group * rows, HEAD_DIM), BF16),
                pltpu.VMEM((n_tp, rows, q_cols), BF16),
                pltpu.VMEM((n_tp, rows, q_cols), BF16),
                dma((len(operands),)),
                pltpu.VMEM((1, width), F32),
                dma((steps, 4)),
                dma((steps, 4)),
                dma((steps, 4)),
                dma((steps, 4)),
                dma((n_sp * n_tp,)),
                dma((n_sp * n_tp,)),
                dma((n_tp + 2, n_sp)),
                dma((n_tp + 2, n_sp)),
                dma((n_tp,)),
                dma((n_tp,)),
            ],
            compiler_params=pltpu.CompilerParams(
                collective_id=0, has_side_effects=True, vmem_limit_bytes=60 * 2**20
            ),
        )(*operands)

    in_specs = (
        P(("grp", "dp"), ("sp", "tp"), None),
        P(("grp", "dp"), None),
        P(("grp", "dp"), "sp", None),
        P(),
        P("sp", "tp"),
        P("sp", "tp"),
        P("sp", "tp"),
        P(),
        P(None, "tp"),
        P(None, "tp"),
        P(None, "tp"),
        P(),
        P(),
        P("tp"),
        P(),
        P(),
    )
    out_specs = P(("grp", "dp"), ("sp", "tp"), None)
    return jax.shard_map(
        on_device, mesh=mesh, in_specs=in_specs, out_specs=out_specs, check_vma=False
    )
```
